32 devices in a mesh: fs: 4 (over y, x), tp: 8 (over z, core).
Axes of the slice: x: 2, y: 2, z: 4, core: 2. Of those that a mesh axis runs over, the one named last changes fastest.
Arguments:
- tokens: bfloat16 [4096, 2048], P(('fs', 'tp')), may hold values from -6 to 6
- norm_gain: float32 [2048], replicated, may hold values from 0.1 to 1.9
- gate_weight: bfloat16 [2048, 5632], P('fs', 'tp'), may hold values from -0.125 to 0.125
- up_weight: bfloat16 [2048, 5632], P('fs', 'tp'), may hold values from -0.125 to 0.125
- down_weight: bfloat16 [5632, 2048], P('tp', 'fs'), may hold values from -0.078125 to 0.078125
Outputs:
- mixed: bfloat16 [4096, 2048], P(('fs', 'tp'))
The draws below stay inside these ranges and needn't reach their ends.
All inputs are finite; a program needn't handle non-finite values.
Results may differ from the reference program's by a relative error of at most 0.0065.
Values may be sent and summed in bfloat16 or wider, within the bound.
A program may use at most 128 MiB of HBM per device.

```python
import jax
import jax.numpy as jnp
from jax import lax

D = 2048
FF = 5632
TOK_DEV = 128
TOKENS = 4096


def shard_levels(stream_key, extent, pieces, low, high):
    factor_of = 1.0
    for dim, blocks in pieces:
        draws = jax.random.uniform(jax.random.fold_in(jax.random.fold_in(stream_key, 6), dim), (blocks,), jnp.float32, low / len(pieces), high / len(pieces))
        factor_of = factor_of * jnp.repeat(jnp.exp(draws), extent[dim] // blocks).reshape((-1,) + (1,) * (len(extent) - 1 - dim))
    return factor_of


def centred(key, dims, scale, limit, cuts=(), held_as=jnp.bfloat16):
    loudness = shard_levels(key, dims, cuts, -0.22, 0.18) if cuts else 1.0
    entries = jax.random.normal(key, dims, jnp.float32) * scale * loudness
    return jnp.minimum(jnp.maximum(entries, -limit), limit).astype(held_as)


def setup_inputs(seed: int = 0) -> dict:
    streams_of = jax.random.split(jax.random.key(seed), 6)
    return {
        "tokens": centred(streams_of[0], (TOKENS, D), 1.0, 6.0, ((0, 32),)),
        "norm_gain": jnp.clip(1.0 + 0.18 * jax.random.normal(streams_of[1], (D,), jnp.float32), 0.1, 1.9),
        "gate_weight": centred(streams_of[2], (D, FF), D ** -0.5, 0.125, ((0, 4), (1, 8))),
        "up_weight": centred(streams_of[3], (D, FF), D ** -0.5, 0.125, ((0, 4), (1, 8))),
        "down_weight": centred(streams_of[4], (FF, D), FF ** -0.5, 0.078125, ((0, 8), (1, 4))),
    }


eps_floor = 0.05

def reference(tokens, norm_gain, gate_weight, up_weight, down_weight):
    blocks = tokens.reshape(-1, TOK_DEV, D)

    def one_block(rows):
        values = rows.astype(jnp.float32)
        factor = lax.rsqrt(lax.optimization_barrier(jnp.mean(values * values, axis=-1, keepdims=True)) + eps_floor)
        normed = (values * factor * norm_gain).astype(jnp.bfloat16)
        gate = jnp.dot(normed, gate_weight, preferred_element_type=jnp.float32)
        upper = jnp.dot(normed, up_weight, preferred_element_type=jnp.float32)
        hidden = (jax.nn.silu(gate) * upper).astype(jnp.bfloat16)
        return jnp.dot(hidden, down_weight, preferred_element_type=jnp.float32).astype(jnp.bfloat16)
    return lax.map(one_block, blocks).reshape(TOKENS, D)
```

```python
import functools
import math

import jax
import jax.numpy as jnp
from jax import lax
from jax.experimental import pallas as pl
from jax.experimental.pallas import tpu as pltpu

eps_floor = 0.05
MESH = pl.DeviceIdType.MESH
F32 = jnp.float32
BF16 = jnp.bfloat16


def kernel(Y, X, Z, C, tok, gain, gw, uw, dw, out, nrm, Wg, Wu, Wd, acc_g, acc_u, hid,
           sib_s, sib_r, rs_s, rs_r, out_acc,
           w_send, w_recv, t_send, t_recv, ts_send, ts_recv, p_send, p_recv, q_send, q_recv):
    F = Y * X
    f = lax.axis_index("fs")
    t = lax.axis_index("tp")
    y, x = f // X, f % X
    z, c = t // C, t % C
    rows, D = tok.shape
    K = gw.shape[0]
    H = gw.shape[1]
    N = dw.shape[1]
    tile = 2 if Z % 2 == 0 else 1

    def fs_at(j, i):
        return lax.rem(y + j, Y) * X + lax.rem(x + i, X)

    def tp_at(zz, cc):
        return zz * C + cc

    sib = lax.rem(c + 1, C)

    barrier = pltpu.get_barrier_semaphore()
    peers = [{"fs": fs_at(0, i)} for i in range(1, X)] + [{"fs": fs_at(j, 0)} for j in range(1, Y)]
    peers += [{"tp": tp_at(lax.rem(z + r, Z), c)} for r in range(1, Z)]
    if C > 1:
        peers += [{"tp": tp_at(z, sib)}]
    for peer in peers:
        pl.semaphore_signal(barrier, inc=1, device_id=peer, device_id_type=MESH)

    values = tok[...].astype(F32)
    factor = lax.rsqrt(jnp.mean(values * values, axis=-1, keepdims=True) + eps_floor)
    nrm[c, z] = (values * factor * gain[...]).astype(BF16)
    pl.semaphore_wait(barrier, len(peers))

    mats = ((gw, Wg), (uw, Wu), (dw, Wd))
    w_copies = []

    def half(ref, h):
        n = ref.shape[0] // 2
        return ref.at[pl.ds(h * n, n)]

    def piece(m, h, j, i):
        own, held = mats[m]
        return half(own, h) if (j, i) == (0, 0) else half(held.at[fs_at(j, i)], h)

    def w_copy(m, h, j, i, dj, di):
        k = len(w_copies)
        slot = ((j - dj) % Y) * X + (i - di) % X
        cp = pltpu.make_async_remote_copy(
            src_ref=piece(m, h, j, i), dst_ref=half(mats[m][1].at[fs_at(j, i)], h),
            send_sem=w_send.at[k], recv_sem=w_recv.at[m, h, slot],
            device_id={"fs": fs_at(dj, di)}, device_id_type=MESH)
        cp.start()
        w_copies.append(cp)

    def w_wait(m, h, j, i):
        ref = half(mats[m][1].at[fs_at(j, i)], h)
        pltpu.make_async_copy(ref, ref, w_recv.at[m, h, j * X + i]).wait()

    def phase_one(ms):
        for m in ms:
            for i in range(1, X):
                w_copy(m, 0, 0, 0, 0, i)
            for j in range(1, Y):
                w_copy(m, 1, 0, 0, j, 0)

    def phase_own(ms):
        for m in ms:
            for i in range(1, X):
                w_copy(m, 1, 0, 0, 0, i)
            for j in range(1, Y):
                w_copy(m, 0, 0, 0, j, 0)

    def phase_relay(ms):
        for m in ms:
            for i in range(1, X):
                w_wait(m, 0, 0, i)
                for j in range(1, Y):
                    w_copy(m, 0, 0, i, j, 0)
            for j in range(1, Y):
                w_wait(m, 1, j, 0)
                for i in range(1, X):
                    w_copy(m, 1, j, 0, 0, i)

    def wait_cross(ms):
        for m in ms:
            for i in range(1, X):
                w_wait(m, 1, 0, i)
            for j in range(1, Y):
                w_wait(m, 0, j, 0)

    def wait_diag(ms):
        for m in ms:
            for j in range(1, Y):
                for i in range(1, X):
                    w_wait(m, 0, j, i)
                    w_wait(m, 1, j, i)

    def tok_chain(direction, s):
        src = z - s if direction == 0 else z + s
        dst = z + 1 if direction == 0 else z - 1
        ok = jnp.logical_and(src >= 0, dst < Z) if direction == 0 else jnp.logical_and(src < Z, dst >= 0)
        src, dst = jnp.clip(src, 0, Z - 1), jnp.clip(dst, 0, Z - 1)
        cp = pltpu.make_async_remote_copy(
            src_ref=nrm.at[c, src], dst_ref=nrm.at[c, src],
            send_sem=t_send.at[direction, s], recv_sem=t_recv.at[direction, s],
            device_id={"tp": tp_at(dst, c)}, device_id_type=MESH)
        return cp, ok

    def tok_sib(zz):
        return pltpu.make_async_remote_copy(
            src_ref=nrm.at[c, zz], dst_ref=nrm.at[c, zz],
            send_sem=ts_send.at[zz], recv_sem=ts_recv.at[zz],
            device_id={"tp": tp_at(z, sib)}, device_id_type=MESH)

    def tok_start(s):
        for direction in range(2):
            cp, ok = tok_chain(direction, s)
            pl.when(ok)(cp.start)

    def tok_arrive(s):
        for direction in range(2):
            src = z - s if direction == 0 else z + s
            there = src >= 0 if direction == 0 else src < Z
            src = jnp.clip(src, 0, Z - 1)

            @pl.when(there)
            def _():
                pltpu.make_async_copy(nrm.at[c, src], nrm.at[c, src], t_recv.at[direction, s - 1]).wait()
                if C > 1:
                    tok_sib(src).start()

            if s < Z - 1:
                cp, ok = tok_chain(direction, s)
                pl.when(ok)(cp.start)

    phase_one((0, 1))
    tok_start(0)
    if C > 1:
        tok_sib(z).start()
    phase_own((0, 1))
    if Z > 1:
        tok_arrive(1)
    phase_relay((0, 1))
    for s in range(2, Z):
        tok_arrive(s)
    wait_cross((0, 1))
    phase_one((2,))
    phase_own((2,))
    if C > 1:
        for zz in range(Z):
            ref = nrm.at[sib, zz]
            pltpu.make_async_copy(ref, ref, ts_recv.at[zz]).wait()

    near = [(0, 0)] + [(0, i) for i in range(1, X)] + [(j, 0) for j in range(1, Y)]
    far = [(j, i) for j in range(1, Y) for i in range(1, X)]
    mrows = tile * rows
    per_core = Z // tile

    def products(n, group):
        cc, zt = n // per_core, n % per_core
        g = u = None
        for j, i in group:
            own = (j, i) == (0, 0)
            o = fs_at(j, i)
            a = nrm[cc, pl.ds(zt * tile, tile), :, pl.ds(pl.multiple_of(o * K, K), K)].reshape(mrows, K)
            wg = gw[...] if own else Wg[o]
            wu = uw[...] if own else Wu[o]
            pg = jnp.dot(a, wg, preferred_element_type=F32)
            pu = jnp.dot(a, wu, preferred_element_type=F32)
            g, u = (pg, pu) if g is None else (g + pg, u + pu)
        return g, u

    @pl.loop(0, C * per_core)
    def _(n):
        g, u = products(n, near)
        acc_g[n] = g
        acc_u[n] = u

    wait_diag((0, 1))

    @pl.loop(0, C * per_core)
    def _(n):
        g, u = products(n, far)
        g, u = g + acc_g[n], u + acc_u[n]
        hid[n // per_core, pl.ds((n % per_core) * tile, tile)] = (
            (jax.nn.silu(g) * u).astype(BF16).reshape(tile, rows, H))

    rs_copies = []

    def down_chunk(q, j, i):
        own = (j, i) == (0, 0)
        o = fs_at(j, i)
        cols = pl.ds(pl.multiple_of(o * N, N), N)
        w = (lambda: dw[...]) if own else (lambda: Wd[o])
        if C > 1:
            sib_s[q] = jnp.dot(hid[sib].reshape(Z * rows, H), w(),
                               preferred_element_type=F32).astype(BF16).reshape(Z, rows, N)
            cp = pltpu.make_async_remote_copy(
                src_ref=sib_s.at[q], dst_ref=sib_r.at[q], send_sem=p_send.at[q], recv_sem=p_recv.at[q],
                device_id={"tp": tp_at(z, sib)}, device_id_type=MESH)
            cp.start()
        for r in list(range(1, Z)) + [0]:
            zz = lax.rem(z + r, Z)
            part = jnp.dot(hid[c, zz], w(), preferred_element_type=F32)
            if r == 1 or Z == 1:
                if C > 1:
                    cp.wait_recv()
            if C > 1:
                part = part + sib_r[q, zz].astype(F32)
            if r == 0:
                out_acc[:, cols] = part
            else:
                rs_s[q, r - 1] = part.astype(BF16)
                pltpu.make_async_remote_copy(
                    src_ref=rs_s.at[q, r - 1], dst_ref=rs_r.at[q, r - 1],
                    send_sem=q_send.at[q], recv_sem=q_recv.at[q],
                    device_id={"tp": tp_at(zz, c)}, device_id_type=MESH).start()
        if C > 1:
            rs_copies.append(cp)

    down_chunk(0, 0, 0)
    phase_relay((2,))
    wait_cross((2,))
    q = 1
    for j, i in near[1:]:
        down_chunk(q, j, i)
        q += 1
    wait_diag((2,))
    for j, i in far:
        down_chunk(q, j, i)
        q += 1

    for q, (j, i) in enumerate(near + far):
        cols = pl.ds(pl.multiple_of(fs_at(j, i) * N, N), N)
        total = out_acc[:, cols]
        if Z > 1:
            pltpu.make_async_copy(rs_r.at[q], rs_r.at[q], q_recv.at[q]).wait()
            for r in range(Z - 1):
                total = total + rs_r[q, r].astype(F32)
        out[:, cols] = total.astype(BF16)

    for cp in w_copies:
        cp.wait_send()
    for s in range(Z - 1):
        for direction in range(2):
            cp, ok = tok_chain(direction, s)
            pl.when(ok)(cp.wait_send)
    if C > 1:
        for zz in range(Z):
            tok_sib(zz).wait_send()
        for cp in rs_copies:
            cp.wait_send()
    if Z > 1:
        for q in range(F):
            pltpu.make_async_copy(rs_s.at[q], rs_s.at[q], q_send.at[q]).wait()


def local(sizes, tokens, norm_gain, gate_weight, up_weight, down_weight):
    Y, X, Z, C = sizes
    F = Y * X
    rows, D = tokens.shape
    K, H = gate_weight.shape
    N = down_weight.shape[1]
    tile = 2 if Z % 2 == 0 else 1
    n_w = 3 * ((X - 1) + (Y - 1) * X + (Y - 1) + (X - 1) * Y)
    vmem = pl.BlockSpec(memory_space=pltpu.VMEM)
    dma = pltpu.SemaphoreType.DMA
    hops = max(Z - 1, 1)
    return pl.pallas_call(
        functools.partial(kernel, Y, X, Z, C),
        out_shape=jax.ShapeDtypeStruct((rows, D), BF16),
        in_specs=[vmem] * 5,
        out_specs=vmem,
        scratch_shapes=[
            pltpu.VMEM((C, Z, rows, D), BF16),
            pltpu.VMEM((F, K, H), BF16),
            pltpu.VMEM((F, K, H), BF16),
            pltpu.VMEM((F, H, N), BF16),
            pltpu.VMEM((C * Z // tile, tile * rows, H), F32),
            pltpu.VMEM((C * Z // tile, tile * rows, H), F32),
            pltpu.VMEM((C, Z, rows, H), BF16),
            pltpu.VMEM((F, Z, rows, N), BF16),
            pltpu.VMEM((F, Z, rows, N), BF16),
            pltpu.VMEM((F, hops, rows, N), BF16),
            pltpu.VMEM((F, hops, rows, N), BF16),
            pltpu.VMEM((rows, D), F32),
            dma((max(n_w, 1),)), dma((3, 2, F)),
            dma((2, Z)), dma((2, Z)), dma((Z,)), dma((Z,)),
            dma((F,)), dma((F,)), dma((F,)), dma((F,)),
        ],
        compiler_params=pltpu.CompilerParams(
            collective_id=0, has_side_effects=True, vmem_limit_bytes=60 * 1024 * 1024),
    )(tokens, norm_gain.reshape(1, D), gate_weight, up_weight, down_weight)


def solution(mesh):
    fs, tp = mesh.shape["fs"], mesh.shape["tp"]
    X = max(n for n in range(1, math.isqrt(fs) + 1) if fs % n == 0)
    C = 2 if tp % 2 == 0 else 1
    from jax.sharding import PartitionSpec as P
    return jax.shard_map(
        functools.partial(local, (fs // X, X, tp // C, C)),
        mesh=mesh,
        in_specs=(P(("fs", "tp"), None), P(), P("fs", "tp"), P("fs", "tp"), P("tp", "fs")),
        out_specs=P(("fs", "tp"), None),
        check_vma=False,
    )
```

```python
import functools
import math

import jax
import jax.numpy as jnp
from jax import lax
from jax.experimental import pallas as pl
from jax.experimental.pallas import tpu as pltpu

eps_floor = 0.05
MESH = pl.DeviceIdType.MESH
F32 = jnp.float32
BF16 = jnp.bfloat16


def kernel(Y, X, Z, C, tok, gain, gw, uw, dw, out, nrm, Wg, Wu, Wd, acc_g, acc_u, hid,
           sib_s, sib_r, rs_s, rs_r, part, w_local,
           w_send, w_recv, t_send, t_recv, ts_send, ts_recv, p_send, p_recv, q_send, q_recv):
    F = Y * X
    f = lax.axis_index("fs")
    t = lax.axis_index("tp")
    y, x = f // X, f % X
    z, c = t // C, t % C
    rows, D = tok.shape
    H, K = gw.shape
    N = dw.shape[1]
    tile = 2 if Z % 2 == 0 else 1

    def fs_at(j, i):
        return lax.rem(y + j, Y) * X + lax.rem(x + i, X)

    def tp_at(zz, cc):
        return zz * C + cc

    sib = lax.rem(c + 1, C)

    barrier = pltpu.get_barrier_semaphore()
    peers = [{"fs": fs_at(0, i)} for i in range(1, X)] + [{"fs": fs_at(j, 0)} for j in range(1, Y)]
    if C > 1:
        peers += [{"tp": tp_at(z, sib)}]

    def greet(peer):
        pl.semaphore_signal(barrier, inc=1, device_id=peer, device_id_type=MESH)

    for peer in peers:
        greet(peer)
    below, above = jnp.maximum(z - 1, 0), jnp.minimum(z + 1, Z - 1)
    pl.when(z > 0)(lambda: greet({"tp": tp_at(below, c)}))
    pl.when(z < Z - 1)(lambda: greet({"tp": tp_at(above, c)}))

    mats = ((gw, Wg), (uw, Wu), (dw, Wd))
    own_copies = [pltpu.make_async_copy(ref, held.at[f], w_local.at[m]) for m, (ref, held) in enumerate(mats)]
    for cp in own_copies:
        cp.start()

    values = tok[...].astype(F32)
    factor = lax.rsqrt(jnp.mean(values * values, axis=-1, keepdims=True) + eps_floor)
    nrm[c, z] = (values * factor * gain[...]).astype(BF16)
    pl.semaphore_wait(barrier, len(peers) + (z > 0).astype(jnp.int32) + (z < Z - 1).astype(jnp.int32))
    for cp in own_copies:
        cp.wait()

    w_copies = []

    def half(ref, h):
        n = ref.shape[0] // 2
        return ref.at[pl.ds(h * n, n)]

    def piece(m, h, j, i):
        return half(mats[m][1].at[fs_at(j, i)], h)

    def w_copy(m, h, j, i, dj, di):
        k = len(w_copies)
        slot = ((j - dj) % Y) * X + (i - di) % X
        cp = pltpu.make_async_remote_copy(
            src_ref=piece(m, h, j, i), dst_ref=half(mats[m][1].at[fs_at(j, i)], h),
            send_sem=w_send.at[k], recv_sem=w_recv.at[m, h, slot],
            device_id={"fs": fs_at(dj, di)}, device_id_type=MESH)
        cp.start()
        w_copies.append(cp)

    def w_wait(m, h, j, i):
        ref = half(mats[m][1].at[fs_at(j, i)], h)
        pltpu.make_async_copy(ref, ref, w_recv.at[m, h, j * X + i]).wait()

    def phase_one(ms):
        for m in ms:
            for i in range(1, X):
                w_copy(m, 0, 0, 0, 0, i)
            for j in range(1, Y):
                w_copy(m, 1, 0, 0, j, 0)

    def phase_own(ms):
        for m in ms:
            for i in range(1, X):
                w_copy(m, 1, 0, 0, 0, i)
            for j in range(1, Y):
                w_copy(m, 0, 0, 0, j, 0)

    def phase_relay(ms):
        for m in ms:
            for i in range(1, X):
                w_wait(m, 0, 0, i)
                for j in range(1, Y):
                    w_copy(m, 0, 0, i, j, 0)
            for j in range(1, Y):
                w_wait(m, 1, j, 0)
                for i in range(1, X):
                    w_copy(m, 1, j, 0, 0, i)

    def wait_cross(ms):
        for m in ms:
            for i in range(1, X):
                w_wait(m, 1, 0, i)
            for j in range(1, Y):
                w_wait(m, 0, j, 0)

    def wait_diag(ms):
        for m in ms:
            for j in range(1, Y):
                for i in range(1, X):
                    w_wait(m, 0, j, i)
                    w_wait(m, 1, j, i)

    def tok_chain(direction, s):
        src = z - s if direction == 0 else z + s
        dst = z + 1 if direction == 0 else z - 1
        ok = jnp.logical_and(src >= 0, dst < Z) if direction == 0 else jnp.logical_and(src < Z, dst >= 0)
        src, dst = jnp.clip(src, 0, Z - 1), jnp.clip(dst, 0, Z - 1)
        cp = pltpu.make_async_remote_copy(
            src_ref=nrm.at[c, src], dst_ref=nrm.at[c, src],
            send_sem=t_send.at[direction, s], recv_sem=t_recv.at[direction, s],
            device_id={"tp": tp_at(dst, c)}, device_id_type=MESH)
        return cp, ok

    def tok_sib(zz):
        return pltpu.make_async_remote_copy(
            src_ref=nrm.at[c, zz], dst_ref=nrm.at[c, zz],
            send_sem=ts_send.at[zz], recv_sem=ts_recv.at[zz],
            device_id={"tp": tp_at(z, sib)}, device_id_type=MESH)

    def tok_start(s):
        for direction in range(2):
            cp, ok = tok_chain(direction, s)
            pl.when(ok)(cp.start)

    def tok_arrive(s):
        for direction in range(2):
            src = z - s if direction == 0 else z + s
            there = src >= 0 if direction == 0 else src < Z
            src = jnp.clip(src, 0, Z - 1)

            @pl.when(there)
            def _():
                pltpu.make_async_copy(nrm.at[c, src], nrm.at[c, src], t_recv.at[direction, s - 1]).wait()
                if C > 1:
                    tok_sib(src).start()

            if s < Z - 1:
                cp, ok = tok_chain(direction, s)
                pl.when(ok)(cp.start)

    phase_one((0, 1))
    tok_start(0)
    if C > 1:
        tok_sib(z).start()
    phase_own((0, 1))
    if Z > 1:
        tok_arrive(1)
    phase_relay((0, 1))
    for s in range(2, Z):
        tok_arrive(s)
    wait_cross((0, 1))
    phase_one((2,))
    phase_own((2,))
    if C > 1:
        for zz in range(Z):
            ref = nrm.at[sib, zz]
            pltpu.make_async_copy(ref, ref, ts_recv.at[zz]).wait()

    near = [(0, 0)] + [(0, i) for i in range(1, X)] + [(j, 0) for j in range(1, Y)]
    far = [(j, i) for j in range(1, Y) for i in range(1, X)]
    mrows = tile * rows
    per_core = Z // tile

    def products(n, group):
        cc, zt = n // per_core, n % per_core
        g = u = None
        for j, i in group:
            o = fs_at(j, i)
            a = nrm[cc, pl.ds(zt * tile, tile), :, pl.ds(pl.multiple_of(o * K, K), K)].reshape(mrows, K)
            pg = lax.dot_general(a, Wg[o], (((1,), (1,)), ((), ())), preferred_element_type=F32)
            pu = lax.dot_general(a, Wu[o], (((1,), (1,)), ((), ())), preferred_element_type=F32)
            g, u = (pg, pu) if g is None else (g + pg, u + pu)
        return g, u

    @pl.loop(0, C * per_core)
    def _(n):
        g, u = products(n, near)
        acc_g[n] = g
        acc_u[n] = u

    wait_diag((0, 1))

    @pl.loop(0, C * per_core)
    def _(n):
        g, u = products(n, far)
        g, u = g + acc_g[n], u + acc_u[n]
        hid[n // per_core, pl.ds((n % per_core) * tile, tile)] = (
            (jax.nn.silu(g) * u).astype(BF16).reshape(tile, rows, H))

    sib_copies = []

    def sum_copy(q, direction, d):
        to = above if direction == 0 else below
        return pltpu.make_async_remote_copy(
            src_ref=rs_s.at[q, d], dst_ref=rs_r.at[q, direction, d],
            send_sem=q_send.at[q, d], recv_sem=q_recv.at[q, direction, d],
            device_id={"tp": tp_at(to, c)}, device_id_type=MESH)

    def sum_wait(q, direction, d):
        ref = rs_r.at[q, direction, d]
        pltpu.make_async_copy(ref, ref, q_recv.at[q, direction, d]).wait()

    def down_chunk(q, j, i):
        o = fs_at(j, i)
        if C > 1:
            sib_s[q] = jnp.dot(hid[sib].reshape(Z * rows, H), Wd[o],
                               preferred_element_type=F32).astype(BF16).reshape(Z, rows, N)
            cp = pltpu.make_async_remote_copy(
                src_ref=sib_s.at[q], dst_ref=sib_r.at[q], send_sem=p_send.at[q], recv_sem=p_recv.at[q],
                device_id={"tp": tp_at(z, sib)}, device_id_type=MESH)
            cp.start()
            sib_copies.append(cp)
        part[q] = jnp.dot(hid[c].reshape(Z * rows, H), Wd[o],
                          preferred_element_type=F32).reshape(Z, rows, N)
        if C > 1:
            cp.wait_recv()

            @pl.loop(0, Z)
            def _(d):
                part[q, d] = part[q, d] + sib_r[q, d].astype(F32)

        for direction, first, order in ((0, z == 0, range(Z - 1, 0, -1)), (1, z == Z - 1, range(Z - 1))):
            @pl.when(first)
            def _():
                for d in order:
                    rs_s[q, d] = part[q, d].astype(BF16)
                    sum_copy(q, direction, d).start()

    def sum_relay(q):
        for k in range(Z - 1):
            for direction, d in ((0, Z - 1 - k), (1, k)):
                ok = jnp.logical_and(z > 0, z < d) if direction == 0 else jnp.logical_and(z < Z - 1, z > d)

                @pl.when(ok)
                def _():
                    sum_wait(q, direction, d)
                    rs_s[q, d] = (part[q, d] + rs_r[q, direction, d].astype(F32)).astype(BF16)
                    sum_copy(q, direction, d).start()

    def sum_end(q, j, i):
        for direction, there in ((0, z > 0), (1, z < Z - 1)):
            @pl.when(there)
            def _():
                sum_wait(q, direction, z)
                part[q, z] = part[q, z] + rs_r[q, direction, z].astype(F32)

        out[:, pl.ds(pl.multiple_of(fs_at(j, i) * N, N), N)] = part[q, z].astype(BF16)

    order = near + far
    down_chunk(0, 0, 0)
    phase_relay((2,))
    sum_relay(0)
    wait_cross((2,))
    for q in range(1, len(order)):
        if q == len(near):
            wait_diag((2,))
        down_chunk(q, *order[q])
        if q > 1:
            sum_relay(q - 1)
    if len(order) > 1:
        sum_relay(len(order) - 1)
    for q in range(len(order)):
        sum_end(q, *order[q])

    for cp in w_copies:
        cp.wait_send()
    for s in range(Z - 1):
        for direction in range(2):
            cp, ok = tok_chain(direction, s)
            pl.when(ok)(cp.wait_send)
    if C > 1:
        for zz in range(Z):
            tok_sib(zz).wait_send()
        for cp in sib_copies:
            cp.wait_send()
    for q in range(F):
        for d in range(Z):
            pl.when(z != d)(sum_copy(q, 0, d).wait_send)


def local(sizes, tokens, norm_gain, gate_weight, up_weight, down_weight):
    Y, X, Z, C = sizes
    F = Y * X
    rows, D = tokens.shape
    gate_weight, up_weight = gate_weight.T, up_weight.T
    H, K = gate_weight.shape
    N = down_weight.shape[1]
    tile = 2 if Z % 2 == 0 else 1
    n_w = 3 * ((X - 1) + (Y - 1) * X + (Y - 1) + (X - 1) * Y)
    vmem = pl.BlockSpec(memory_space=pltpu.VMEM)
    dma = pltpu.SemaphoreType.DMA
    hbm = pl.BlockSpec(memory_space=pl.ANY)
    return pl.pallas_call(
        functools.partial(kernel, Y, X, Z, C),
        out_shape=jax.ShapeDtypeStruct((rows, D), BF16),
        in_specs=[vmem] * 2 + [hbm] * 3,
        out_specs=vmem,
        scratch_shapes=[
            pltpu.VMEM((C, Z, rows, D), BF16),
            pltpu.VMEM((F, H, K), BF16),
            pltpu.VMEM((F, H, K), BF16),
            pltpu.VMEM((F, H, N), BF16),
            pltpu.VMEM((C * Z // tile, tile * rows, H), F32),
            pltpu.VMEM((C * Z // tile, tile * rows, H), F32),
            pltpu.VMEM((C, Z, rows, H), BF16),
            pltpu.VMEM((F, Z, rows, N), BF16),
            pltpu.VMEM((F, Z, rows, N), BF16),
            pltpu.VMEM((F, Z, rows, N), BF16),
            pltpu.VMEM((F, 2, Z, rows, N), BF16),
            pltpu.VMEM((F, Z, rows, N), F32),
            dma((3,)),
            dma((max(n_w, 1),)), dma((3, 2, F)),
            dma((2, Z)), dma((2, Z)), dma((Z,)), dma((Z,)),
            dma((F,)), dma((F,)), dma((F, Z)), dma((F, 2, Z)),
        ],
        compiler_params=pltpu.CompilerParams(
            collective_id=0, has_side_effects=True, vmem_limit_bytes=60 * 1024 * 1024),
    )(tokens, norm_gain.reshape(1, D), gate_weight, up_weight, down_weight)


def solution(mesh):
    fs, tp = mesh.shape["fs"], mesh.shape["tp"]
    X = max(n for n in range(1, math.isqrt(fs) + 1) if fs % n == 0)
    C = 2 if tp % 2 == 0 else 1
    from jax.sharding import PartitionSpec as P
    return jax.shard_map(
        functools.partial(local, (fs // X, X, tp // C, C)),
        mesh=mesh,
        in_specs=(P(("fs", "tp"), None), P(), P("fs", "tp"), P("fs", "tp"), P("tp", "fs")),
        out_specs=P(("fs", "tp"), None),
        check_vma=False,
    )
```

```python
import functools
import math

import jax
import jax.numpy as jnp
from jax import lax
from jax.experimental import pallas as pl
from jax.experimental.pallas import tpu as pltpu

eps_floor = 0.05
MESH = pl.DeviceIdType.MESH
F32 = jnp.float32
BF16 = jnp.bfloat16


def kernel(Y, X, Z, C, cuts, tok, gain, gw, uw, dw, out, nrm, Wg, Wu, Wd, acc_g, acc_u, hid,
           sib_s, sib_r, rs_s, rs_r, part, w_local,
           w_send, w_recv, t_send, t_recv, ts_send, ts_recv, p_send, p_recv, q_send, q_recv):
    F = Y * X
    f = lax.axis_index("fs")
    t = lax.axis_index("tp")
    y, x = f // X, f % X
    z, c = t // C, t % C
    rows, D = tok.shape
    H, K = gw.shape
    N = dw.shape[1] // cuts
    tile = 2 if Z % 2 == 0 else 1

    def fs_at(j, i):
        return lax.rem(y + j, Y) * X + lax.rem(x + i, X)

    def tp_at(zz, cc):
        return zz * C + cc

    sib = lax.rem(c + 1, C)

    barrier = pltpu.get_barrier_semaphore()
    peers = [{"fs": fs_at(0, i)} for i in range(1, X)] + [{"fs": fs_at(j, 0)} for j in range(1, Y)]
    if C > 1:
        peers += [{"tp": tp_at(z, sib)}]

    def greet(peer):
        pl.semaphore_signal(barrier, inc=1, device_id=peer, device_id_type=MESH)

    for peer in peers:
        greet(peer)
    below, above = jnp.maximum(z - 1, 0), jnp.minimum(z + 1, Z - 1)
    pl.when(z > 0)(lambda: greet({"tp": tp_at(below, c)}))
    pl.when(z < Z - 1)(lambda: greet({"tp": tp_at(above, c)}))

    mats = ((gw, Wg), (uw, Wu), (dw, Wd))
    own_copies = [pltpu.make_async_copy(ref, held.at[f], w_local.at[m]) for m, (ref, held) in enumerate(mats)]
    for cp in own_copies:
        cp.start()

    values = tok[...].astype(F32)
    factor = lax.rsqrt(jnp.mean(values * values, axis=-1, keepdims=True) + eps_floor)
    nrm[c, z] = (values * factor * gain[...]).astype(BF16)
    pl.semaphore_wait(barrier, len(peers) + (z > 0).astype(jnp.int32) + (z < Z - 1).astype(jnp.int32))
    for cp in own_copies:
        cp.wait()

    w_copies = []

    def piece(m, h, j, i):
        held = mats[m][1].at[fs_at(j, i)]
        if m == 2 and cuts == 2:
            return held.at[:, pl.ds(h * N, N)]
        n = held.shape[0] // 2
        return held.at[pl.ds(h * n, n)]

    def w_copy(m, h, j, i, dj, di):
        k = len(w_copies)
        slot = ((j - dj) % Y) * X + (i - di) % X
        cp = pltpu.make_async_remote_copy(
            src_ref=piece(m, h, j, i), dst_ref=piece(m, h, j, i),
            send_sem=w_send.at[k], recv_sem=w_recv.at[m, h, slot],
            device_id={"fs": fs_at(dj, di)}, device_id_type=MESH)
        cp.start()
        w_copies.append(cp)

    def w_wait(m, h, j, i):
        ref = piece(m, h, j, i)
        pltpu.make_async_copy(ref, ref, w_recv.at[m, h, j * X + i]).wait()

    def phase_one(ms):
        for m in ms:
            for i in range(1, X):
                w_copy(m, 0, 0, 0, 0, i)
            for j in range(1, Y):
                w_copy(m, 1, 0, 0, j, 0)

    def phase_own(ms):
        for m in ms:
            for i in range(1, X):
                w_copy(m, 1, 0, 0, 0, i)
            for j in range(1, Y):
                w_copy(m, 0, 0, 0, j, 0)

    def phase_relay(ms):
        for m in ms:
            for i in range(1, X):
                w_wait(m, 0, 0, i)
                for j in range(1, Y):
                    w_copy(m, 0, 0, i, j, 0)
            for j in range(1, Y):
                w_wait(m, 1, j, 0)
                for i in range(1, X):
                    w_copy(m, 1, j, 0, 0, i)

    def wait_cross(ms):
        for m in ms:
            for i in range(1, X):
                w_wait(m, 1, 0, i)
            for j in range(1, Y):
                w_wait(m, 0, j, 0)

    def wait_diag(ms):
        for m in ms:
            for j in range(1, Y):
                for i in range(1, X):
                    w_wait(m, 0, j, i)
                    w_wait(m, 1, j, i)

    def tok_chain(direction, s):
        src = z - s if direction == 0 else z + s
        dst = z + 1 if direction == 0 else z - 1
        ok = jnp.logical_and(src >= 0, dst < Z) if direction == 0 else jnp.logical_and(src < Z, dst >= 0)
        src, dst = jnp.clip(src, 0, Z - 1), jnp.clip(dst, 0, Z - 1)
        cp = pltpu.make_async_remote_copy(
            src_ref=nrm.at[c, src], dst_ref=nrm.at[c, src],
            send_sem=t_send.at[direction, s], recv_sem=t_recv.at[direction, s],
            device_id={"tp": tp_at(dst, c)}, device_id_type=MESH)
        return cp, ok

    def tok_sib(zz):
        return pltpu.make_async_remote_copy(
            src_ref=nrm.at[c, zz], dst_ref=nrm.at[c, zz],
            send_sem=ts_send.at[zz], recv_sem=ts_recv.at[zz],
            device_id={"tp": tp_at(z, sib)}, device_id_type=MESH)

    def tok_start(s):
        for direction in range(2):
            cp, ok = tok_chain(direction, s)
            pl.when(ok)(cp.start)

    def tok_arrive(s):
        for direction in range(2):
            src = z - s if direction == 0 else z + s
            there = src >= 0 if direction == 0 else src < Z
            src = jnp.clip(src, 0, Z - 1)

            @pl.when(there)
            def _():
                pltpu.make_async_copy(nrm.at[c, src], nrm.at[c, src], t_recv.at[direction, s - 1]).wait()
                if C > 1:
                    tok_sib(src).start()

            if s < Z - 1:
                cp, ok = tok_chain(direction, s)
                pl.when(ok)(cp.start)

    phase_one((0, 1))
    tok_start(0)
    if C > 1:
        tok_sib(z).start()
    phase_own((0, 1))
    if Z > 1:
        tok_arrive(1)
    phase_relay((0, 1))
    for s in range(2, Z):
        tok_arrive(s)
    wait_cross((0, 1))
    phase_one((2,))
    phase_own((2,))
    if C > 1:
        for zz in range(Z):
            ref = nrm.at[sib, zz]
            pltpu.make_async_copy(ref, ref, ts_recv.at[zz]).wait()

    near = [(0, 0)] + [(0, i) for i in range(1, X)] + [(j, 0) for j in range(1, Y)]
    far = [(j, i) for j in range(1, Y) for i in range(1, X)]
    mrows = tile * rows
    per_core = Z // tile

    def products(n, group):
        cc, zt = n // per_core, n % per_core
        g = u = None
        for j, i in group:
            o = fs_at(j, i)
            a = nrm[cc, pl.ds(zt * tile, tile), :, pl.ds(pl.multiple_of(o * K, K), K)].reshape(mrows, K)
            pg = lax.dot_general(a, Wg[o], (((1,), (1,)), ((), ())), preferred_element_type=F32)
            pu = lax.dot_general(a, Wu[o], (((1,), (1,)), ((), ())), preferred_element_type=F32)
            g, u = (pg, pu) if g is None else (g + pg, u + pu)
        return g, u

    @pl.loop(0, C * per_core)
    def _(n):
        g, u = products(n, near)
        acc_g[n] = g
        acc_u[n] = u

    wait_diag((0, 1))

    @pl.loop(0, C * per_core)
    def _(n):
        g, u = products(n, far)
        g, u = g + acc_g[n], u + acc_u[n]
        hid[n // per_core, pl.ds((n % per_core) * tile, tile)] = (
            (jax.nn.silu(g) * u).astype(BF16).reshape(tile, rows, H))

    sib_copies = []

    def sum_copy(q, direction, d):
        to = above if direction == 0 else below
        return pltpu.make_async_remote_copy(
            src_ref=rs_s.at[q, d], dst_ref=rs_r.at[q, direction, d],
            send_sem=q_send.at[q, d], recv_sem=q_recv.at[q, direction, d],
            device_id={"tp": tp_at(to, c)}, device_id_type=MESH)

    def sum_wait(q, direction, d):
        ref = rs_r.at[q, direction, d]
        pltpu.make_async_copy(ref, ref, q_recv.at[q, direction, d]).wait()

    units = []

    def down(new):
        qs = list(range(len(units), len(units) + len(new)))
        units.extend(new)

        def weight(q):
            j, i, h = units[q]
            return Wd[fs_at(j, i), :, h * N:(h + 1) * N]

        copies = []
        if C > 1:
            for q in qs:
                sib_s[q] = jnp.dot(hid[sib].reshape(Z * rows, H), weight(q),
                                   preferred_element_type=F32).astype(BF16).reshape(Z, rows, N)
                cp = pltpu.make_async_remote_copy(
                    src_ref=sib_s.at[q], dst_ref=sib_r.at[q], send_sem=p_send.at[q], recv_sem=p_recv.at[q],
                    device_id={"tp": tp_at(z, sib)}, device_id_type=MESH)
                cp.start()
                copies.append(cp)
        for q in qs:
            part[q] = jnp.dot(hid[c].reshape(Z * rows, H), weight(q),
                              preferred_element_type=F32).reshape(Z, rows, N)
        for q, cp in zip(qs, copies):
            cp.wait_recv()

            @pl.loop(0, Z)
            def _(d):
                part[q, d] = part[q, d] + sib_r[q, d].astype(F32)
        sib_copies.extend(copies)

        for direction, first, order in ((0, z == 0, range(Z - 1, 0, -1)), (1, z == Z - 1, range(Z - 1))):
            @pl.when(first)
            def _():
                for d in order:
                    for q in qs:
                        rs_s[q, d] = part[q, d].astype(BF16)
                        sum_copy(q, direction, d).start()
        return qs

    low = 2 * z < Z

    def sum_step(q, direction, d, ok):
        @pl.when(ok)
        def _():
            sum_wait(q, direction, d)
            rs_s[q, d] = (part[q, d] + rs_r[q, direction, d].astype(F32)).astype(BF16)
            sum_copy(q, direction, d).start()

    def sum_near(qs):
        for d in range(Z - 1, 0, -1):
            for q in qs:
                sum_step(q, 0, d, jnp.logical_and(jnp.logical_and(z > 0, z < d), low))
        for d in range(Z - 1):
            for q in qs:
                sum_step(q, 1, d, jnp.logical_and(jnp.logical_and(z < Z - 1, z > d), jnp.logical_not(low)))

    def sum_far(qs):
        for d in range(Z - 1, 0, -1):
            for q in qs:
                sum_step(q, 0, d, jnp.logical_and(z < d, jnp.logical_not(low)))
        for d in range(Z - 1):
            for q in qs:
                sum_step(q, 1, d, jnp.logical_and(z > d, low))

    def sum_end(q):
        j, i, h = units[q]
        for direction, there in ((0, z > 0), (1, z < Z - 1)):
            @pl.when(there)
            def _():
                sum_wait(q, direction, z)
                part[q, z] = part[q, z] + rs_r[q, direction, z].astype(F32)

        out[:, pl.ds(pl.multiple_of((fs_at(j, i) * cuts + h) * N, N), N)] = part[q, z].astype(BF16)

    in_row = [(0, i) for i in range(1, X)]
    in_col = [(j, 0) for j in range(1, Y)]
    both = range(cuts)
    early = [(j, i, 0) for j, i in in_row] + [(j, i, 1) for j, i in in_col] if cuts == 2 else []
    mid = [(j, i, h) for h in both for j, i in in_row + in_col if (j, i, h) not in early]
    qa = down([(0, 0, h) for h in both])
    phase_relay((2,))
    qb = down(early)
    sum_near(qa)
    wait_cross((2,))
    qc = down(mid)
    sum_near(qb)
    sum_far(qa)
    wait_diag((2,))
    qd = down([(j, i, h) for j, i in far for h in both])
    sum_near(qc)
    sum_far(qb)
    sum_near(qd)
    sum_far(qc)
    sum_far(qd)
    for q in range(len(units)):
        sum_end(q)

    for cp in w_copies:
        cp.wait_send()
    for s in range(Z - 1):
        for direction in range(2):
            cp, ok = tok_chain(direction, s)
            pl.when(ok)(cp.wait_send)
    if C > 1:
        for zz in range(Z):
            tok_sib(zz).wait_send()
        for cp in sib_copies:
            cp.wait_send()
    for q in range(len(units)):
        for d in range(Z):
            pl.when(z != d)(sum_copy(q, 0, d).wait_send)


def local(sizes, tokens, norm_gain, gate_weight, up_weight, down_weight):
    Y, X, Z, C = sizes
    F = Y * X
    rows, D = tokens.shape
    gate_weight, up_weight = gate_weight.T, up_weight.T
    H, K = gate_weight.shape
    cuts = 2 if down_weight.shape[1] % 256 == 0 else 1
    N = down_weight.shape[1] // cuts
    U = F * cuts
    tile = 2 if Z % 2 == 0 else 1
    n_w = 3 * ((X - 1) + (Y - 1) * X + (Y - 1) + (X - 1) * Y)
    vmem = pl.BlockSpec(memory_space=pltpu.VMEM)
    dma = pltpu.SemaphoreType.DMA
    hbm = pl.BlockSpec(memory_space=pl.ANY)
    return pl.pallas_call(
        functools.partial(kernel, Y, X, Z, C, cuts),
        out_shape=jax.ShapeDtypeStruct((rows, D), BF16),
        in_specs=[vmem] * 2 + [hbm] * 3,
        out_specs=vmem,
        scratch_shapes=[
            pltpu.VMEM((C, Z, rows, D), BF16),
            pltpu.VMEM((F, H, K), BF16),
            pltpu.VMEM((F, H, K), BF16),
            pltpu.VMEM((F, H, N * cuts), BF16),
            pltpu.VMEM((C * Z // tile, tile * rows, H), F32),
            pltpu.VMEM((C * Z // tile, tile * rows, H), F32),
            pltpu.VMEM((C, Z, rows, H), BF16),
            pltpu.VMEM((U, Z, rows, N), BF16),
            pltpu.VMEM((U, Z, rows, N), BF16),
            pltpu.VMEM((U, Z, rows, N), BF16),
            pltpu.VMEM((U, 2, Z, rows, N), BF16),
            pltpu.VMEM((U, Z, rows, N), F32),
            dma((3,)),
            dma((max(n_w, 1),)), dma((3, 2, F)),
            dma((2, Z)), dma((2, Z)), dma((Z,)), dma((Z,)),
            dma((U,)), dma((U,)), dma((U, Z)), dma((U, 2, Z)),
        ],
        compiler_params=pltpu.CompilerParams(
            collective_id=0, has_side_effects=True, vmem_limit_bytes=60 * 1024 * 1024),
    )(tokens, norm_gain.reshape(1, D), gate_weight, up_weight, down_weight)


def solution(mesh):
    fs, tp = mesh.shape["fs"], mesh.shape["tp"]
    X = max(n for n in range(1, math.isqrt(fs) + 1) if fs % n == 0)
    C = 2 if tp % 2 == 0 else 1
    from jax.sharding import PartitionSpec as P
    return jax.shard_map(
        functools.partial(local, (fs // X, X, tp // C, C)),
        mesh=mesh,
        in_specs=(P(("fs", "tp"), None), P(), P("fs", "tp"), P("fs", "tp"), P("tp", "fs")),
        out_specs=P(("fs", "tp"), None),
        check_vma=False,
    )
```

```python
import functools
import math

import jax
import jax.numpy as jnp
from jax import lax
from jax.experimental import pallas as pl
from jax.experimental.pallas import tpu as pltpu

eps_floor = 0.05
MESH = pl.DeviceIdType.MESH
F32 = jnp.float32
BF16 = jnp.bfloat16


def kernel(Y, X, Z, C, cuts, tok, gain, gw, uw, dw, out, nrm, Wg, Wu, Wd, acc_g, acc_u, hid,
           sib_s, sib_r, rs_s, rs_r, part, w_local,
           w_send, w_recv, t_send, t_recv, ts_send, ts_recv, p_send, p_recv, q_send, q_recv):
    F = Y * X
    f = lax.axis_index("fs")
    t = lax.axis_index("tp")
    y, x = f // X, f % X
    z, c = t // C, t % C
    rows, D = tok.shape
    H, K = gw.shape
    N = dw.shape[1] // cuts
    tile = 2 if Z % 2 == 0 else 1

    def fs_at(j, i):
        return lax.rem(y + j, Y) * X + lax.rem(x + i, X)

    def tp_at(zz, cc):
        return zz * C + cc

    sib = lax.rem(c + 1, C)

    barrier = pltpu.get_barrier_semaphore()
    peers = [{"fs": fs_at(0, i)} for i in range(1, X)] + [{"fs": fs_at(j, 0)} for j in range(1, Y)]
    if C > 1:
        peers += [{"tp": tp_at(z, sib)}]

    def greet(peer):
        pl.semaphore_signal(barrier, inc=1, device_id=peer, device_id_type=MESH)

    for peer in peers:
        greet(peer)
    below, above = jnp.maximum(z - 1, 0), jnp.minimum(z + 1, Z - 1)
    pl.when(z > 0)(lambda: greet({"tp": tp_at(below, c)}))
    pl.when(z < Z - 1)(lambda: greet({"tp": tp_at(above, c)}))

    mats = ((gw, Wg), (uw, Wu), (dw, Wd))
    own_copies = [pltpu.make_async_copy(ref, held.at[f], w_local.at[m]) for m, (ref, held) in enumerate(mats)]
    for cp in own_copies:
        cp.start()

    values = tok[...].astype(F32)
    factor = lax.rsqrt(jnp.mean(values * values, axis=-1, keepdims=True) + eps_floor)
    nrm[c, z] = (values * factor * gain[...]).astype(BF16)
    pl.semaphore_wait(barrier, len(peers) + (z > 0).astype(jnp.int32) + (z < Z - 1).astype(jnp.int32))
    for cp in own_copies:
        cp.wait()

    w_copies = []

    def piece(m, h, j, i):
        held = mats[m][1].at[fs_at(j, i)]
        if m == 2 and cuts == 2:
            return held.at[:, pl.ds(h * N, N)]
        n = held.shape[0] // 2
        return held.at[pl.ds(h * n, n)]

    def w_copy(m, h, j, i, dj, di):
        k = len(w_copies)
        slot = ((j - dj) % Y) * X + (i - di) % X
        cp = pltpu.make_async_remote_copy(
            src_ref=piece(m, h, j, i), dst_ref=piece(m, h, j, i),
            send_sem=w_send.at[k], recv_sem=w_recv.at[m, h, slot],
            device_id={"fs": fs_at(dj, di)}, device_id_type=MESH)
        cp.start()
        w_copies.append(cp)

    def w_wait(m, h, j, i):
        ref = piece(m, h, j, i)
        pltpu.make_async_copy(ref, ref, w_recv.at[m, h, j * X + i]).wait()

    def phase_one(ms):
        for m in ms:
            for i in range(1, X):
                w_copy(m, 0, 0, 0, 0, i)
            for j in range(1, Y):
                w_copy(m, 1, 0, 0, j, 0)

    def phase_own(ms):
        for m in ms:
            for i in range(1, X):
                w_copy(m, 1, 0, 0, 0, i)
            for j in range(1, Y):
                w_copy(m, 0, 0, 0, j, 0)

    def phase_relay(ms):
        for m in ms:
            for i in range(1, X):
                w_wait(m, 0, 0, i)
                for j in range(1, Y):
                    w_copy(m, 0, 0, i, j, 0)
            for j in range(1, Y):
                w_wait(m, 1, j, 0)
                for i in range(1, X):
                    w_copy(m, 1, j, 0, 0, i)

    def wait_cross(ms):
        for m in ms:
            for i in range(1, X):
                w_wait(m, 1, 0, i)
            for j in range(1, Y):
                w_wait(m, 0, j, 0)

    def wait_diag(ms):
        for m in ms:
            for j in range(1, Y):
                for i in range(1, X):
                    w_wait(m, 0, j, i)
                    w_wait(m, 1, j, i)

    def tok_chain(direction, s):
        src = z - s if direction == 0 else z + s
        dst = z + 1 if direction == 0 else z - 1
        ok = jnp.logical_and(src >= 0, dst < Z) if direction == 0 else jnp.logical_and(src < Z, dst >= 0)
        src, dst = jnp.clip(src, 0, Z - 1), jnp.clip(dst, 0, Z - 1)
        cp = pltpu.make_async_remote_copy(
            src_ref=nrm.at[c, src], dst_ref=nrm.at[c, src],
            send_sem=t_send.at[direction, s], recv_sem=t_recv.at[direction, s],
            device_id={"tp": tp_at(dst, c)}, device_id_type=MESH)
        return cp, ok

    def tok_sib(zz):
        return pltpu.make_async_remote_copy(
            src_ref=nrm.at[c, zz], dst_ref=nrm.at[c, zz],
            send_sem=ts_send.at[zz], recv_sem=ts_recv.at[zz],
            device_id={"tp": tp_at(z, sib)}, device_id_type=MESH)

    def tok_start(s):
        for direction in range(2):
            cp, ok = tok_chain(direction, s)
            pl.when(ok)(cp.start)

    def tok_arrive(s):
        for direction in range(2):
            src = z - s if direction == 0 else z + s
            there = src >= 0 if direction == 0 else src < Z
            src = jnp.clip(src, 0, Z - 1)

            @pl.when(there)
            def _():
                pltpu.make_async_copy(nrm.at[c, src], nrm.at[c, src], t_recv.at[direction, s - 1]).wait()
                if C > 1:
                    tok_sib(src).start()

            if s < Z - 1:
                cp, ok = tok_chain(direction, s)
                pl.when(ok)(cp.start)

    phase_one((0, 1))
    tok_start(0)
    if C > 1:
        tok_sib(z).start()
    phase_own((0, 1))
    if Z > 1:
        tok_arrive(1)
    phase_relay((0, 1))
    for s in range(2, Z):
        tok_arrive(s)
    wait_cross((0, 1))
    phase_one((2,))
    phase_own((2,))
    if C > 1:
        for zz in range(Z):
            ref = nrm.at[sib, zz]
            pltpu.make_async_copy(ref, ref, ts_recv.at[zz]).wait()

    near = [(0, 0)] + [(0, i) for i in range(1, X)] + [(j, 0) for j in range(1, Y)]
    far = [(j, i) for j in range(1, Y) for i in range(1, X)]
    mrows = tile * rows
    per_core = Z // tile

    def product(n, held, group):
        cc, zt = n // per_core, n % per_core
        total = None
        for j, i in group:
            o = fs_at(j, i)
            a = nrm[cc, pl.ds(zt * tile, tile), :, pl.ds(pl.multiple_of(o * K, K), K)].reshape(mrows, K)
            p = lax.dot_general(a, held[o], (((1,), (1,)), ((), ())), preferred_element_type=F32)
            total = p if total is None else total + p
        return total

    @pl.loop(0, C * per_core)
    def _(n):
        acc_g[n] = product(n, Wg, near)
        acc_u[n] = product(n, Wu, near)

    wait_diag((0,))

    @pl.loop(0, C * per_core)
    def _(n):
        g = acc_g[n]
        if far:
            g = g + product(n, Wg, far)
        acc_g[n] = jax.nn.silu(g)

    wait_diag((1,))

    @pl.loop(0, C * per_core)
    def _(n):
        u = acc_u[n]
        if far:
            u = u + product(n, Wu, far)
        hid[n // per_core, pl.ds((n % per_core) * tile, tile)] = (acc_g[n] * u).astype(BF16).reshape(tile, rows, H)

    sib_copies = []

    def sum_copy(q, direction, d):
        to = above if direction == 0 else below
        return pltpu.make_async_remote_copy(
            src_ref=rs_s.at[q, d], dst_ref=rs_r.at[q, direction, d],
            send_sem=q_send.at[q, d], recv_sem=q_recv.at[q, direction, d],
            device_id={"tp": tp_at(to, c)}, device_id_type=MESH)

    def sum_wait(q, direction, d):
        ref = rs_r.at[q, direction, d]
        pltpu.make_async_copy(ref, ref, q_recv.at[q, direction, d]).wait()

    units = []

    def down(new):
        qs = list(range(len(units), len(units) + len(new)))
        units.extend(new)

        def weight(q):
            j, i, h = units[q]
            return Wd[fs_at(j, i), :, h * N:(h + 1) * N]

        copies = []
        if C > 1:
            for q in qs:
                sib_s[q] = jnp.dot(hid[sib].reshape(Z * rows, H), weight(q),
                                   preferred_element_type=F32).astype(BF16).reshape(Z, rows, N)
                cp = pltpu.make_async_remote_copy(
                    src_ref=sib_s.at[q], dst_ref=sib_r.at[q], send_sem=p_send.at[q], recv_sem=p_recv.at[q],
                    device_id={"tp": tp_at(z, sib)}, device_id_type=MESH)
                cp.start()
                copies.append(cp)
        for q in qs:
            part[q] = jnp.dot(hid[c].reshape(Z * rows, H), weight(q),
                              preferred_element_type=F32).reshape(Z, rows, N)
        for q, cp in zip(qs, copies):
            cp.wait_recv()

            @pl.loop(0, Z)
            def _(d):
                part[q, d] = part[q, d] + sib_r[q, d].astype(F32)
        sib_copies.extend(copies)

        for direction, first, order in ((0, z == 0, range(Z - 1, 0, -1)), (1, z == Z - 1, range(Z - 1))):
            @pl.when(first)
            def _():
                for d in order:
                    for q in qs:
                        rs_s[q, d] = part[q, d].astype(BF16)
                        sum_copy(q, direction, d).start()
        return qs

    low = 2 * z < Z

    def sum_step(q, direction, d, ok):
        @pl.when(ok)
        def _():
            sum_wait(q, direction, d)
            rs_s[q, d] = (part[q, d] + rs_r[q, direction, d].astype(F32)).astype(BF16)
            sum_copy(q, direction, d).start()

    def sum_near(qs):
        for d in range(Z - 1, 0, -1):
            for q in qs:
                sum_step(q, 0, d, jnp.logical_and(jnp.logical_and(z > 0, z < d), low))
        for d in range(Z - 1):
            for q in qs:
                sum_step(q, 1, d, jnp.logical_and(jnp.logical_and(z < Z - 1, z > d), jnp.logical_not(low)))

    def sum_far(qs):
        for d in range(Z - 1, 0, -1):
            for q in qs:
                sum_step(q, 0, d, jnp.logical_and(z < d, jnp.logical_not(low)))
        for d in range(Z - 1):
            for q in qs:
                sum_step(q, 1, d, jnp.logical_and(z > d, low))

    def sum_end(q):
        j, i, h = units[q]
        for direction, there in ((0, z > 0), (1, z < Z - 1)):
            @pl.when(there)
            def _():
                sum_wait(q, direction, z)
                part[q, z] = part[q, z] + rs_r[q, direction, z].astype(F32)

        out[:, pl.ds(pl.multiple_of((fs_at(j, i) * cuts + h) * N, N), N)] = part[q, z].astype(BF16)

    in_row = [(0, i) for i in range(1, X)]
    in_col = [(j, 0) for j in range(1, Y)]
    both = range(cuts)
    early = [(j, i, 0) for j, i in in_row] + [(j, i, 1) for j, i in in_col] if cuts == 2 else []
    mid = [(j, i, h) for h in both for j, i in in_row + in_col if (j, i, h) not in early]
    qa = [q for h in both for q in down([(0, 0, h)])]
    phase_relay((2,))
    qb = down(early)
    sum_near(qa)
    wait_cross((2,))
    qc = down(mid)
    sum_near(qb)
    sum_far(qa)
    wait_diag((2,))
    qd = down([(j, i, h) for j, i in far for h in both])
    sum_near(qc)
    sum_far(qb)
    for q in qa + qb:
        sum_end(q)
    sum_far(qc)
    sum_near(qd)
    for q in qc:
        sum_end(q)
    sum_far(qd)
    for q in qd:
        sum_end(q)

    for cp in w_copies:
        cp.wait_send()
    for s in range(Z - 1):
        for direction in range(2):
            cp, ok = tok_chain(direction, s)
            pl.when(ok)(cp.wait_send)
    if C > 1:
        for zz in range(Z):
            tok_sib(zz).wait_send()
        for cp in sib_copies:
            cp.wait_send()
    for q in range(len(units)):
        for d in range(Z):
            pl.when(z != d)(sum_copy(q, 0, d).wait_send)


def local(sizes, tokens, norm_gain, gate_weight, up_weight, down_weight):
    Y, X, Z, C = sizes
    F = Y * X
    rows, D = tokens.shape
    gate_weight, up_weight = gate_weight.T, up_weight.T
    H, K = gate_weight.shape
    cuts = 2 if down_weight.shape[1] % 256 == 0 else 1
    N = down_weight.shape[1] // cuts
    U = F * cuts
    tile = 2 if Z % 2 == 0 else 1
    n_w = 3 * ((X - 1) + (Y - 1) * X + (Y - 1) + (X - 1) * Y)
    vmem = pl.BlockSpec(memory_space=pltpu.VMEM)
    dma = pltpu.SemaphoreType.DMA
    hbm = pl.BlockSpec(memory_space=pl.ANY)
    return pl.pallas_call(
        functools.partial(kernel, Y, X, Z, C, cuts),
        out_shape=pltpu.VMEM((rows, D), BF16),
        in_specs=[vmem] * 2 + [hbm] * 3,
        out_specs=vmem,
        scratch_shapes=[
            pltpu.VMEM((C, Z, rows, D), BF16),
            pltpu.VMEM((F, H, K), BF16),
            pltpu.VMEM((F, H, K), BF16),
            pltpu.VMEM((F, H, N * cuts), BF16),
            pltpu.VMEM((C * Z // tile, tile * rows, H), F32),
            pltpu.VMEM((C * Z // tile, tile * rows, H), F32),
            pltpu.VMEM((C, Z, rows, H), BF16),
            pltpu.VMEM((U, Z, rows, N), BF16),
            pltpu.VMEM((U, Z, rows, N), BF16),
            pltpu.VMEM((U, Z, rows, N), BF16),
            pltpu.VMEM((U, 2, Z, rows, N), BF16),
            pltpu.VMEM((U, Z, rows, N), F32),
            dma((3,)),
            dma((max(n_w, 1),)), dma((3, 2, F)),
            dma((2, Z)), dma((2, Z)), dma((Z,)), dma((Z,)),
            dma((U,)), dma((U,)), dma((U, Z)), dma((U, 2, Z)),
        ],
        compiler_params=pltpu.CompilerParams(
            collective_id=0, has_side_effects=True, vmem_limit_bytes=60 * 1024 * 1024),
    )(tokens, norm_gain.reshape(1, D), gate_weight, up_weight, down_weight)


def solution(mesh):
    fs, tp = mesh.shape["fs"], mesh.shape["tp"]
    X = max(n for n in range(1, math.isqrt(fs) + 1) if fs % n == 0)
    C = 2 if tp % 2 == 0 else 1
    from jax.sharding import PartitionSpec as P
    return jax.shard_map(
        functools.partial(local, (fs // X, X, tp // C, C)),
        mesh=mesh,
        in_specs=(P(("fs", "tp"), None), P(), P("fs", "tp"), P("fs", "tp"), P("tp", "fs")),
        out_specs=P(("fs", "tp"), None),
        check_vma=False,
    )
```

```python
import functools
import math

import jax
import jax.numpy as jnp
from jax import lax
from jax.experimental import pallas as pl
from jax.experimental.pallas import tpu as pltpu

eps_floor = 0.05
MESH = pl.DeviceIdType.MESH
F32 = jnp.float32
BF16 = jnp.bfloat16


def kernel(Y, X, Z, C, cuts, tok, gain, gw, uw, dw, out, nrm, Wg, Wu, Wd, acc_g, acc_u, hid,
           sib_s, sib_r, rs_s, rs_r, part, w_local,
           w_send, w_recv, t_send, t_recv, ts_send, ts_recv, p_send, p_recv, q_send, q_recv):
    F = Y * X
    f = lax.axis_index("fs")
    t = lax.axis_index("tp")
    y, x = f // X, f % X
    z, c = t // C, t % C
    rows, D = tok.shape
    H, K = gw.shape
    N = dw.shape[1] // cuts
    tile = 2 if Z % 2 == 0 else 1

    def fs_at(j, i):
        return lax.rem(y + j, Y) * X + lax.rem(x + i, X)

    def tp_at(zz, cc):
        return zz * C + cc

    sib = lax.rem(c + 1, C)

    barrier = pltpu.get_barrier_semaphore()
    peers = [{"fs": fs_at(0, i)} for i in range(1, X)] + [{"fs": fs_at(j, 0)} for j in range(1, Y)]
    if C > 1:
        peers += [{"tp": tp_at(z, sib)}]

    def greet(peer):
        pl.semaphore_signal(barrier, inc=1, device_id=peer, device_id_type=MESH)

    for peer in peers:
        greet(peer)
    below, above = jnp.maximum(z - 1, 0), jnp.minimum(z + 1, Z - 1)
    pl.when(z > 0)(lambda: greet({"tp": tp_at(below, c)}))
    pl.when(z < Z - 1)(lambda: greet({"tp": tp_at(above, c)}))

    mats = ((gw, Wg), (uw, Wu), (dw, Wd))
    own_copies = [pltpu.make_async_copy(ref, held.at[f], w_local.at[m]) for m, (ref, held) in enumerate(mats)]
    for cp in own_copies:
        cp.start()

    pl.semaphore_wait(barrier, len(peers) + (z > 0).astype(jnp.int32) + (z < Z - 1).astype(jnp.int32))
    for cp in own_copies:
        cp.wait()

    w_copies = []

    def piece(m, h, j, i):
        held = mats[m][1].at[fs_at(j, i)]
        if m == 2 and cuts == 2:
            return held.at[:, pl.ds(h * N, N)]
        n = held.shape[0] // 2
        return held.at[pl.ds(h * n, n)]

    def w_copy(m, h, j, i, dj, di):
        k = len(w_copies)
        slot = ((j - dj) % Y) * X + (i - di) % X
        cp = pltpu.make_async_remote_copy(
            src_ref=piece(m, h, j, i), dst_ref=piece(m, h, j, i),
            send_sem=w_send.at[k], recv_sem=w_recv.at[m, h, slot],
            device_id={"fs": fs_at(dj, di)}, device_id_type=MESH)
        cp.start()
        w_copies.append(cp)

    def w_wait(m, h, j, i):
        ref = piece(m, h, j, i)
        pltpu.make_async_copy(ref, ref, w_recv.at[m, h, j * X + i]).wait()

    def phase_one(ms):
        for m in ms:
            for i in range(1, X):
                w_copy(m, 0, 0, 0, 0, i)
            for j in range(1, Y):
                w_copy(m, 1, 0, 0, j, 0)

    def phase_own(ms):
        for m in ms:
            for i in range(1, X):
                w_copy(m, 1, 0, 0, 0, i)
            for j in range(1, Y):
                w_copy(m, 0, 0, 0, j, 0)

    def phase_relay(ms):
        for m in ms:
            for i in range(1, X):
                w_wait(m, 0, 0, i)
                for j in range(1, Y):
                    w_copy(m, 0, 0, i, j, 0)
            for j in range(1, Y):
                w_wait(m, 1, j, 0)
                for i in range(1, X):
                    w_copy(m, 1, j, 0, 0, i)

    def wait_cross(ms):
        for m in ms:
            for i in range(1, X):
                w_wait(m, 1, 0, i)
            for j in range(1, Y):
                w_wait(m, 0, j, 0)

    def wait_diag(ms):
        for m in ms:
            for j in range(1, Y):
                for i in range(1, X):
                    w_wait(m, 0, j, i)
                    w_wait(m, 1, j, i)

    def tok_chain(direction, s):
        src = z - s if direction == 0 else z + s
        dst = z + 1 if direction == 0 else z - 1
        ok = jnp.logical_and(src >= 0, dst < Z) if direction == 0 else jnp.logical_and(src < Z, dst >= 0)
        src, dst = jnp.clip(src, 0, Z - 1), jnp.clip(dst, 0, Z - 1)
        cp = pltpu.make_async_remote_copy(
            src_ref=nrm.at[c, src], dst_ref=nrm.at[c, src],
            send_sem=t_send.at[direction, s], recv_sem=t_recv.at[direction, s],
            device_id={"tp": tp_at(dst, c)}, device_id_type=MESH)
        return cp, ok

    def tok_sib(zz):
        return pltpu.make_async_remote_copy(
            src_ref=nrm.at[c, zz], dst_ref=nrm.at[c, zz],
            send_sem=ts_send.at[zz], recv_sem=ts_recv.at[zz],
            device_id={"tp": tp_at(z, sib)}, device_id_type=MESH)

    def tok_start(s):
        for direction in range(2):
            cp, ok = tok_chain(direction, s)
            pl.when(ok)(cp.start)

    def tok_arrive(s):
        for direction in range(2):
            src = z - s if direction == 0 else z + s
            there = src >= 0 if direction == 0 else src < Z
            src = jnp.clip(src, 0, Z - 1)

            @pl.when(there)
            def _():
                pltpu.make_async_copy(nrm.at[c, src], nrm.at[c, src], t_recv.at[direction, s - 1]).wait()
                if C > 1:
                    tok_sib(src).start()

            if s < Z - 1:
                cp, ok = tok_chain(direction, s)
                pl.when(ok)(cp.start)

    phase_one((0, 1))
    values = tok[...].astype(F32)
    factor = lax.rsqrt(jnp.mean(values * values, axis=-1, keepdims=True) + eps_floor)
    nrm[c, z] = (values * factor * gain[...]).astype(BF16)
    tok_start(0)
    if C > 1:
        tok_sib(z).start()
    phase_own((0, 1))
    if Z > 1:
        tok_arrive(1)
    phase_relay((0, 1))
    for s in range(2, Z):
        tok_arrive(s)
    wait_cross((0, 1))
    phase_one((2,))
    phase_own((2,))
    if C > 1:
        for zz in range(Z):
            ref = nrm.at[sib, zz]
            pltpu.make_async_copy(ref, ref, ts_recv.at[zz]).wait()

    near = [(0, 0)] + [(0, i) for i in range(1, X)] + [(j, 0) for j in range(1, Y)]
    far = [(j, i) for j in range(1, Y) for i in range(1, X)]
    mrows = tile * rows
    per_core = Z // tile

    def product(n, held, group):
        cc, zt = n // per_core, n % per_core
        total = None
        for j, i in group:
            o = fs_at(j, i)
            a = nrm[cc, pl.ds(zt * tile, tile), :, pl.ds(pl.multiple_of(o * K, K), K)].reshape(mrows, K)
            p = lax.dot_general(a, held[o], (((1,), (1,)), ((), ())), preferred_element_type=F32)
            total = p if total is None else total + p
        return total

    @pl.loop(0, C * per_core)
    def _(n):
        acc_g[n] = product(n, Wg, near)
        acc_u[n] = product(n, Wu, near)

    wait_diag((0,))

    @pl.loop(0, C * per_core)
    def _(n):
        g = acc_g[n]
        if far:
            g = g + product(n, Wg, far)
        acc_g[n] = jax.nn.silu(g)

    wait_diag((1,))

    @pl.loop(0, C * per_core)
    def _(n):
        u = acc_u[n]
        if far:
            u = u + product(n, Wu, far)
        hid[n // per_core, pl.ds((n % per_core) * tile, tile)] = (acc_g[n] * u).astype(BF16).reshape(tile, rows, H)

    sib_copies = []

    def sum_copy(q, direction, d):
        to = above if direction == 0 else below
        return pltpu.make_async_remote_copy(
            src_ref=rs_s.at[q, d], dst_ref=rs_r.at[q, direction, d],
            send_sem=q_send.at[q, d], recv_sem=q_recv.at[q, direction, d],
            device_id={"tp": tp_at(to, c)}, device_id_type=MESH)

    def sum_wait(q, direction, d):
        ref = rs_r.at[q, direction, d]
        pltpu.make_async_copy(ref, ref, q_recv.at[q, direction, d]).wait()

    units = []

    def down(new):
        qs = list(range(len(units), len(units) + len(new)))
        units.extend(new)

        def weight(q):
            j, i, h = units[q]
            return Wd[fs_at(j, i), :, h * N:(h + 1) * N]

        copies = []
        if C > 1:
            for q in qs:
                sib_s[q] = jnp.dot(hid[sib].reshape(Z * rows, H), weight(q),
                                   preferred_element_type=F32).astype(BF16).reshape(Z, rows, N)
                cp = pltpu.make_async_remote_copy(
                    src_ref=sib_s.at[q], dst_ref=sib_r.at[q], send_sem=p_send.at[q], recv_sem=p_recv.at[q],
                    device_id={"tp": tp_at(z, sib)}, device_id_type=MESH)
                cp.start()
                copies.append(cp)
        for q in qs:
            part[q] = jnp.dot(hid[c].reshape(Z * rows, H), weight(q),
                              preferred_element_type=F32).reshape(Z, rows, N)
        for q, cp in zip(qs, copies):
            cp.wait_recv()

            @pl.loop(0, Z)
            def _(d):
                part[q, d] = part[q, d] + sib_r[q, d].astype(F32)
        sib_copies.extend(copies)

        for direction, first, order in ((0, z == 0, range(Z - 1, 0, -1)), (1, z == Z - 1, range(Z - 1))):
            @pl.when(first)
            def _():
                for d in order:
                    for q in qs:
                        rs_s[q, d] = part[q, d].astype(BF16)
                        sum_copy(q, direction, d).start()
        return qs

    low = 2 * z < Z

    def sum_step(q, direction, d, ok):
        @pl.when(ok)
        def _():
            sum_wait(q, direction, d)
            rs_s[q, d] = (part[q, d] + rs_r[q, direction, d].astype(F32)).astype(BF16)
            sum_copy(q, direction, d).start()

    def sum_near(qs):
        for d in range(Z - 1, 0, -1):
            for q in qs:
                sum_step(q, 0, d, jnp.logical_and(jnp.logical_and(z > 0, z < d), low))
        for d in range(Z - 1):
            for q in qs:
                sum_step(q, 1, d, jnp.logical_and(jnp.logical_and(z < Z - 1, z > d), jnp.logical_not(low)))

    def sum_far(qs):
        for d in range(Z - 1, 0, -1):
            for q in qs:
                sum_step(q, 0, d, jnp.logical_and(z < d, jnp.logical_not(low)))
        for d in range(Z - 1):
            for q in qs:
                sum_step(q, 1, d, jnp.logical_and(z > d, low))

    def sum_end(q):
        j, i, h = units[q]
        for direction, there in ((0, z > 0), (1, z < Z - 1)):
            @pl.when(there)
            def _():
                sum_wait(q, direction, z)
                part[q, z] = part[q, z] + rs_r[q, direction, z].astype(F32)

        out[:, pl.ds(pl.multiple_of((fs_at(j, i) * cuts + h) * N, N), N)] = part[q, z].astype(BF16)

    in_row = [(0, i) for i in range(1, X)]
    in_col = [(j, 0) for j in range(1, Y)]
    both = range(cuts)
    early = [(j, i, 0) for j, i in in_row] + [(j, i, 1) for j, i in in_col] if cuts == 2 else []
    mid = [(j, i, h) for h in both for j, i in in_row + in_col if (j, i, h) not in early]
    qa = [q for h in both for q in down([(0, 0, h)])]
    phase_relay((2,))
    qb = down(early)
    sum_near(qa)
    wait_cross((2,))
    qc = down(mid)
    sum_near(qb)
    sum_far(qa)
    wait_diag((2,))
    qd = down([(j, i, h) for j, i in far for h in both])
    sum_near(qc)
    sum_far(qb)
    for q in qa + qb:
        sum_end(q)
    sum_far(qc)
    sum_near(qd)
    for q in qc:
        sum_end(q)
    sum_far(qd)
    for q in qd:
        sum_end(q)

    for cp in w_copies:
        cp.wait_send()
    for s in range(Z - 1):
        for direction in range(2):
            cp, ok = tok_chain(direction, s)
            pl.when(ok)(cp.wait_send)
    if C > 1:
        for zz in range(Z):
            tok_sib(zz).wait_send()
        for cp in sib_copies:
            cp.wait_send()
    for q in range(len(units)):
        for d in range(Z):
            pl.when(z != d)(sum_copy(q, 0, d).wait_send)


def local(sizes, tokens, norm_gain, gate_weight, up_weight, down_weight):
    Y, X, Z, C = sizes
    F = Y * X
    rows, D = tokens.shape
    gate_weight, up_weight = gate_weight.T, up_weight.T
    H, K = gate_weight.shape
    cuts = 2 if down_weight.shape[1] % 256 == 0 else 1
    N = down_weight.shape[1] // cuts
    U = F * cuts
    tile = 2 if Z % 2 == 0 else 1
    n_w = 3 * ((X - 1) + (Y - 1) * X + (Y - 1) + (X - 1) * Y)
    vmem = pl.BlockSpec(memory_space=pltpu.VMEM)
    dma = pltpu.SemaphoreType.DMA
    hbm = pl.BlockSpec(memory_space=pl.ANY)
    return pl.pallas_call(
        functools.partial(kernel, Y, X, Z, C, cuts),
        out_shape=pltpu.VMEM((rows, D), BF16),
        in_specs=[vmem] * 2 + [hbm] * 3,
        out_specs=vmem,
        scratch_shapes=[
            pltpu.VMEM((C, Z, rows, D), BF16),
            pltpu.VMEM((F, H, K), BF16),
            pltpu.VMEM((F, H, K), BF16),
            pltpu.VMEM((F, H, N * cuts), BF16),
            pltpu.VMEM((C * Z // tile, tile * rows, H), F32),
            pltpu.VMEM((C * Z // tile, tile * rows, H), F32),
            pltpu.VMEM((C, Z, rows, H), BF16),
            pltpu.VMEM((U, Z, rows, N), BF16),
            pltpu.VMEM((U, Z, rows, N), BF16),
            pltpu.VMEM((U, Z, rows, N), BF16),
            pltpu.VMEM((U, 2, Z, rows, N), BF16),
            pltpu.VMEM((U, Z, rows, N), F32),
            dma((3,)),
            dma((max(n_w, 1),)), dma((3, 2, F)),
            dma((2, Z)), dma((2, Z)), dma((Z,)), dma((Z,)),
            dma((U,)), dma((U,)), dma((U, Z)), dma((U, 2, Z)),
        ],
        compiler_params=pltpu.CompilerParams(
            collective_id=0, has_side_effects=True, vmem_limit_bytes=60 * 1024 * 1024),
    )(tokens, norm_gain.reshape(1, D), gate_weight, up_weight, down_weight)


def solution(mesh):
    fs, tp = mesh.shape["fs"], mesh.shape["tp"]
    X = max(n for n in range(1, math.isqrt(fs) + 1) if fs % n == 0)
    C = 2 if tp % 2 == 0 else 1
    from jax.sharding import PartitionSpec as P
    return jax.shard_map(
        functools.partial(local, (fs // X, X, tp // C, C)),
        mesh=mesh,
        in_specs=(P(("fs", "tp"), None), P(), P("fs", "tp"), P("fs", "tp"), P("tp", "fs")),
        out_specs=P(("fs", "tp"), None),
        check_vma=False,
    )
```
